32 devices in a mesh: rep: 16 (over z, y, core), fs: 2 (over x), tp: 1.
Axes of the slice: x: 2, y: 2, z: 4, core: 2. Of those that a mesh axis runs over, the one named last changes fastest.
Arguments:
- pre_act: bfloat16 [16384, 4096], P('rep', ('fs', 'tp')), may hold values from -6 to 6
- down_weight: bfloat16 [4096, 2048], P(('fs', 'tp')), may hold values from -0.09375 to 0.09375
- cotangent: bfloat16 [16384, 2048], P('rep', ('fs', 'tp')), may hold values from -6 to 6
Outputs:
- grad_pre: bfloat16 [16384, 4096], P('rep', ('fs', 'tp'))
- grad_weight: float32 [4096, 2048], P(('fs', 'tp', 'rep'))
The draws below stay inside these ranges and needn't reach their ends.
All inputs are finite; a program needn't handle non-finite values.
Results may differ from the reference program's by a relative error of at most 0.0029.
Values may be sent and summed in bfloat16 or wider, within the bound.
A program may use at most 128 MiB of HBM per device.

```python
import jax
import jax.numpy as jnp

D = 2048
FF = 4096
TOKENS = 16384


def with_spikes(array, own_key, source, target, parts, factor):
    def block_of(position):
        return (jnp.arange(array.shape[position]) // (array.shape[position] // parts)).reshape((-1,) + (1,) * (array.ndim - 1 - position))

    first = jax.random.permutation(own_key, parts)[block_of(target)]
    other_side = (block_of(target) + parts // 2) % parts
    return jnp.where((block_of(source) == first) | (block_of(source) == other_side), factor * array, array)


def level_of(rng, dims, split, smallest, largest):
    factor_of = 1.0
    for axis_at, blocks in split:
        draws = jax.random.uniform(jax.random.fold_in(jax.random.fold_in(rng, 6), axis_at), (blocks,), jnp.float32, smallest / len(split), largest / len(split))
        factor_of = factor_of * jnp.repeat(jnp.exp(draws), dims[axis_at] // blocks).reshape((-1,) + (1,) * (len(dims) - 1 - axis_at))
    return factor_of


def bell_draw(key, extent, deviation, bound, cuts=(), kind=jnp.bfloat16):
    factor_of = level_of(key, extent, cuts, -0.22, 0.18) if cuts else 1.0
    drawn = jax.random.normal(key, extent, jnp.float32) * deviation * factor_of
    return jnp.minimum(jnp.maximum(drawn, -bound), bound).astype(kind)


def bell_draw_with(stream_key, dims, deviation, most, split, heavy, kind=jnp.bfloat16):
    entries = deviation * jax.random.normal(stream_key, dims, jnp.float32)
    if split:
        entries = entries * level_of(stream_key, dims, split, -0.22, 0.18)
    return jnp.clip(with_spikes(entries, jax.random.fold_in(stream_key, 3), *heavy), -most, most).astype(kind)


def setup_inputs(seed: int = 0) -> dict:
    arg_keys = jax.random.split(jax.random.key(seed), 4)
    pre_act = bell_draw(arg_keys[0], (TOKENS, FF), 1.0, 6.0, ((0, 16), (1, 2)))
    down_weight = bell_draw(arg_keys[1], (FF, D), FF ** -0.5, 0.09375, ((0, 2),))
    cotangent = bell_draw_with(arg_keys[2], (TOKENS, D), 1.0, 6.0, ((0, 16), (1, 2)), (0, 1, 16, 2.0))
    return {"pre_act": pre_act, "down_weight": down_weight, "cotangent": cotangent}


def reference(pre_act, down_weight, cotangent):
    grad_hidden = jnp.dot(cotangent, down_weight.T, preferred_element_type=jnp.float32)
    positive = jnp.maximum(pre_act.astype(jnp.float32), 0.0)
    grad_pre = (grad_hidden * 2.0 * positive).astype(jnp.bfloat16)
    hidden = (positive * positive).astype(jnp.bfloat16)
    summed = jnp.dot(hidden.T, cotangent, preferred_element_type=jnp.float32)
    grad_weight = summed * (1.0 / jnp.sqrt(jnp.float32(TOKENS)))
    return (grad_pre, grad_weight)
```

```python
import functools

import jax
import jax.numpy as jnp
from jax import lax
from jax.experimental import pallas as pl
from jax.experimental.pallas import tpu as pltpu
from jax.sharding import PartitionSpec as P

MESH = pl.DeviceIdType.MESH
CORES, ROWS = 2, 2
F32, BF16 = jnp.float32, jnp.bfloat16


def chunks_of(width, sizes):
    out, at = [], 0
    for s in sizes:
        out.append((at, s))
        at += s
    assert at == width
    return out


def plain(pre_act, down_weight, cotangent):
    whole = lax.all_gather(cotangent, ("fs", "tp"), axis=1, tiled=True)
    grad_hidden = lax.dot_general(
        whole, down_weight, (((1,), (1,)), ((), ())), preferred_element_type=F32
    )
    positive = jnp.maximum(pre_act.astype(F32), 0.0)
    grad_pre = (grad_hidden * 2.0 * positive).astype(BF16)
    hidden = (positive * positive).astype(BF16)
    factor = 1.0 / jnp.sqrt(jnp.float32(pre_act.shape[0] * lax.axis_size("rep")))
    term = lax.dot_general(
        hidden, whole, (((0,), (0,)), ((), ())), preferred_element_type=F32
    )
    summed = lax.psum_scatter(term, "rep", scatter_dimension=0, tiled=True)
    return (grad_pre, summed * factor)


def kernel(
    depth, near, far, factor,
    pre_hbm, w_hbm, cot_hbm, gp_hbm, gw_hbm,
    pre, pre_in, turned, w, cot, grad, gp,
    y_out, y_in, own, z_out, z_in, gw,
    s_local, s_pre_s, s_pre_r, s_near_s, s_near_r, s_x_s, s_x_r, s_fwd_s, s_fwd_r,
    s_y_s, s_y_r, s_z_s, s_z_r, s_gp,
):
    rep, fs, tp = lax.axis_index("rep"), lax.axis_index("fs"), lax.axis_index("tp")
    c, y, z = rep % CORES, (rep // CORES) % ROWS, rep // (CORES * ROWS)
    tokens, half = cot_hbm.shape
    hid = w_hbm.shape[0]
    block = own.shape[1]
    blocks = 2 * depth

    def at(z_, y_, c_, f_):
        return ((z_ * ROWS + y_) * CORES + c_, f_, tp)

    partner, across, beside = at(z, y, 1 - c, fs), at(z, y, c, 1 - fs), at(z, 1 - y, c, fs)

    def remote(src, dst, s, r, to):
        return pltpu.make_async_remote_copy(
            src_ref=src, dst_ref=dst, send_sem=s, recv_sem=r, device_id=to, device_id_type=MESH
        )

    def columns(i, c_):
        y_ = (1 - y) if i < depth else y
        k = (i % depth) * ROWS + y_
        return pl.ds(pl.multiple_of((k * CORES + c_) * block, block), block)

    def local(i, src, dst):
        return pltpu.make_async_copy(src, dst, s_local.at[i])

    loads = [local(0, pre_hbm, pre), local(1, cot_hbm, cot.at[0, pl.ds(0, tokens)]), local(2, w_hbm, w)]
    for l in loads:
        l.start()

    barrier = pltpu.get_barrier_semaphore()
    peers = [partner, across, beside]
    for d in range(1, depth):
        peers.append(at((z + d) % depth, y, c, fs))
    for p in peers:
        pl.semaphore_signal(barrier, inc=1, device_id=p, device_id_type=MESH)
    pl.semaphore_wait(barrier, len(peers))

    x_copies = []
    for q, (a, n) in enumerate(far):
        x_copies.append(remote(
            cot_hbm.at[:, pl.ds(a, n)], cot.at[1, pl.ds(0, tokens), pl.ds(a, n)],
            s_x_s.at[q], s_x_r.at[q], across))
    x_copies[0].start()
    pre_copies = []
    for i in range(blocks):
        pre_copies.append(remote(
            pre_hbm.at[:, columns(i, 1 - c)], pre_in.at[i], s_pre_s.at[i], s_pre_r.at[i], partner))
        pre_copies[-1].start()
    near_copies = []
    for q, (a, n) in enumerate(near):
        near_copies.append(remote(
            cot_hbm.at[:, pl.ds(a, n)], cot.at[0, pl.ds(tokens, tokens), pl.ds(a, n)],
            s_near_s.at[q], s_near_r.at[q], partner))
        near_copies[-1].start()
    for xc in x_copies[1:]:
        xc.start()

    def turn(v):
        p = jnp.maximum(v.astype(F32), 0.0)
        return (p * p).T.astype(BF16)

    strip = 256

    loads[0].wait()
    for i in range(blocks):
        cols = columns(i, c)

        @pl.loop(0, tokens // strip)
        def _(t):
            rows = pl.ds(pl.multiple_of(t * strip, strip), strip)
            turned[pl.ds(i * block, block), rows] = turn(pre[rows, cols])

    loads[1].wait()
    loads[2].wait()
    for pc in pre_copies:
        pc.wait_recv()

    @pl.loop(0, blocks)
    def _(i):
        @pl.loop(0, tokens // strip)
        def _(t):
            rows = pl.ds(pl.multiple_of(t * strip, strip), strip)
            to = pl.ds(pl.multiple_of(tokens + t * strip, strip), strip)
            turned[pl.ds(pl.multiple_of(i * block, block), block), to] = turn(pre_in[i, rows, :])

    tall = 2 * block

    chunks = [(0, a, n) for a, n in near] + [(1, a, n) for a, n in far]

    def span(h, a, n):
        return pl.ds(h * half + a, n)

    def y_copy(j):
        h, a, n = chunks[j]
        s = span(h, a, n)
        return remote(y_out.at[:, :, s], y_in.at[:, :, s], s_y_s.at[j], s_y_r.at[j], beside)

    def z_copy(j, d):
        h, a, n = chunks[j]
        s = span(h, a, n)
        to = (z + d) % depth
        return remote(
            z_out.at[to, :, s], z_in.at[d - 1, :, s],
            s_z_s.at[j * (depth - 1) + d - 1], s_z_r.at[j * (depth - 1) + d - 1], at(to, y, c, fs))

    def fwd_copy(q):
        a, n = far[q]
        return remote(
            cot.at[1, pl.ds(0, tokens), pl.ds(a, n)], cot.at[1, pl.ds(tokens, tokens), pl.ds(a, n)],
            s_fwd_s.at[q], s_fwd_r.at[q], partner)

    def product(j):
        h, a, n = chunks[j]
        s = span(h, a, n)

        def dot(m):
            rows = pl.ds(pl.multiple_of(m * tall, tall), tall)
            return lax.dot_general(
                turned[rows, :], cot[h, :, pl.ds(a, n)], (((1,), (0,)), ((), ())),
                preferred_element_type=F32).reshape(2, block, n)

        @pl.loop(0, depth // 2)
        def _(m):
            y_out[pl.ds(m * 2, 2), :, s] = dot(m).astype(BF16)

        y_copy(j).start()

        @pl.loop(0, depth // 2)
        def _(m):
            own[pl.ds(m * 2, 2), :, s] = dot(m + depth // 2)

    def second(j):
        h, a, n = chunks[j]
        s = span(h, a, n)
        y_copy(j).wait_recv()

        @pl.loop(0, depth)
        def _(k):
            v = own[k, :, s] + y_in[k, :, s].astype(F32)
            own[k, :, s] = v
            z_out[k, :, s] = v.astype(BF16)

        for d in range(1, depth):
            z_copy(j, d).start()

    def last(j):
        h, a, n = chunks[j]
        s = span(h, a, n)
        for d in range(1, depth):
            z_copy(j, d).wait_recv()
        v = own[z, :, s]
        for d in range(depth - 1):
            v = v + z_in[d, :, s].astype(F32)
        place = pl.multiple_of((fs if h == 0 else 1 - fs) * half + a, 128)
        gw[:, pl.ds(place, n)] = v * factor

    tm, tn = 256, 512

    def grad_tile(h, a, n, m, k):
        rows = pl.ds(pl.multiple_of(m * tm, tm), tm)
        outs = pl.ds(pl.multiple_of(k * tn, tn), tn)
        place = pl.multiple_of((fs if h == 0 else 1 - fs) * half + a, 128)
        return rows, outs, lax.dot_general(
            cot[h, rows, pl.ds(a, n)], w[outs, pl.ds(place, n)], (((1,), (1,)), ((), ())),
            preferred_element_type=F32)

    def grad_first():
        @pl.loop(0, tokens // tm)
        def _(m):
            @pl.loop(0, hid // tn)
            def _(k):
                rows, outs, v = grad_tile(0, 0, half, m, k)
                grad[rows, outs] = v

    def gp_copy(m):
        rows = pl.ds(pl.multiple_of(m * tm, tm), tm)
        return pltpu.make_async_copy(gp.at[rows], gp_hbm.at[rows], s_gp.at[m])

    def grad_rest():
        @pl.loop(0, tokens // tm)
        def _(m):
            @pl.loop(0, hid // tn)
            def _(k):
                rows, outs, v = grad_tile(1, 0, half, m, k)
                p = jnp.maximum(pre[rows, outs].astype(F32), 0.0)
                gp[rows, outs] = ((grad[rows, outs] + v) * 2.0 * p).astype(BF16)
            gp_copy(m).start()

    nn, nf = len(near), len(far)
    for q in range(nn):
        near_copies[q].wait_recv()
        product(q)
    grad_first()

    done2 = 0
    done3 = 0
    for q in range(nf):
        while done2 < min(nn + q - 1, (q * (nn + nf)) // nf):
            second(done2)
            done2 += 1
        x_copies[q].wait_recv()
        fwd_copy(q).start()
        fwd_copy(q).wait_recv()
        product(nn + q)
    grad_rest()
    total = nn + nf
    while done2 < total:
        second(done2)
        done2 += 1
        while done3 < done2 - 2:
            last(done3)
            done3 += 1
    while done3 < total:
        last(done3)
        done3 += 1
    out = local(3, gw, gw_hbm)
    out.start()

    for copy in pre_copies + near_copies + x_copies:
        copy.wait_send()
    for q in range(nf):
        fwd_copy(q).wait_send()
    for j in range(total):
        y_copy(j).wait_send()
        for d in range(1, depth):
            z_copy(j, d).wait_send()

    @pl.loop(0, tokens // tm)
    def _(m):
        gp_copy(m).wait()
    out.wait()


def solution(mesh):
    reps, fs, tp = mesh.shape["rep"], mesh.shape["fs"], mesh.shape["tp"]
    depth = reps // (CORES * ROWS)

    def on_device(pre_act, down_weight, cotangent):
        tokens, hid = pre_act.shape
        half = cotangent.shape[1]
        width = down_weight.shape[1]
        block = hid // reps
        if not (fs == 2 and tp == 1 and depth * CORES * ROWS == reps and depth % 2 == 0
                and block % 128 == 0 and half % 1024 == 0 and hid % 512 == 0 and tokens % 256 == 0):
            return plain(pre_act, down_weight, cotangent)
        step = half // 4
        near = chunks_of(half, [step] * 4)
        far = chunks_of(half, [step] * 3 + [step // 2] * 2)
        nn, nf = len(near), len(far)
        total = nn + nf
        factor = 1.0 / float(tokens * reps) ** 0.5
        dma = lambda n: pltpu.SemaphoreType.DMA((n,))
        vm = pltpu.VMEM
        return pl.pallas_call(
            functools.partial(kernel, depth, near, far, factor),
            out_shape=[
                jax.ShapeDtypeStruct((tokens, hid), BF16),
                jax.ShapeDtypeStruct((block, width), F32),
            ],
            in_specs=[pl.BlockSpec(memory_space=pl.ANY)] * 3,
            out_specs=[pl.BlockSpec(memory_space=pl.ANY)] * 2,
            scratch_shapes=[
                vm((tokens, hid), BF16),
                vm((2 * depth, tokens, block), BF16),
                vm((2 * depth * block, 2 * tokens), BF16),
                vm(down_weight.shape, BF16),
                vm((2, 2 * tokens, half), BF16),
                vm((tokens, hid), F32),
                vm((tokens, hid), BF16),
                vm((depth, block, width), BF16),
                vm((depth, block, width), BF16),
                vm((depth, block, width), F32),
                vm((depth, block, width), BF16),
                vm((depth - 1, block, width), BF16),
                vm((block, width), F32),
                dma(4), dma(2 * depth), dma(2 * depth), dma(nn), dma(nn), dma(nf), dma(nf), dma(nf), dma(nf),
                dma(total), dma(total), dma(total * (depth - 1)), dma(total * (depth - 1)),
                dma(tokens // 256),
            ],
            compiler_params=pltpu.CompilerParams(
                collective_id=0, has_side_effects=True, vmem_limit_bytes=66 * 1000 * 1000
            ),
            cost_estimate=pl.CostEstimate(
                flops=8 * tokens * hid * width // 2, bytes_accessed=40 * 1024 * 1024, transcendentals=0),
        )(pre_act, down_weight, cotangent)

    return jax.shard_map(
        on_device,
        mesh=mesh,
        in_specs=(P("rep", ("fs", "tp")), P(("fs", "tp"), None), P("rep", ("fs", "tp"))),
        out_specs=(P("rep", ("fs", "tp")), P(("fs", "tp", "rep"), None)),
        check_vma=False,
    )
```

```python
import functools

import jax
import jax.numpy as jnp
from jax import lax
from jax.experimental import pallas as pl
from jax.experimental.pallas import tpu as pltpu
from jax.sharding import PartitionSpec as P

MESH = pl.DeviceIdType.MESH
CORES, ROWS = 2, 2
F32, BF16 = jnp.float32, jnp.bfloat16


ORDER = (
    "n0 A0 n1 A1",
    "o4 i4 B0 B1",
    "n2 A2 n3 A3",
    "s0 B2 x0 B3",
    "f0 A4 B4 s1",
    "g0 g1 x1 t0",
    "g2 f1 s2 A5",
    "B5 t1 g3 h0",
    "t2 h1 s3 h2",
    "h3 l0 t3 s4",
    "x2 l1 f2 A6",
    "B6 s5 t4 l2",
    "x3 l3 f3 A7",
    "B7 s6 x4 t5",
    "f4 A8 B8 s7",
    "e0 t6 l4 e1",
    "s8 e2 l5 l6",
    "e3 l7 l8",
)


def chunks_of(width, sizes):
    out, at = [], 0
    for s in sizes:
        out.append((at, s))
        at += s
    assert at == width
    return out


def plain(pre_act, down_weight, cotangent):
    whole = lax.all_gather(cotangent, ("fs", "tp"), axis=1, tiled=True)
    grad_hidden = lax.dot_general(
        whole, down_weight, (((1,), (1,)), ((), ())), preferred_element_type=F32
    )
    positive = jnp.maximum(pre_act.astype(F32), 0.0)
    grad_pre = (grad_hidden * 2.0 * positive).astype(BF16)
    hidden = (positive * positive).astype(BF16)
    factor = 1.0 / jnp.sqrt(jnp.float32(pre_act.shape[0] * lax.axis_size("rep")))
    term = lax.dot_general(
        hidden, whole, (((0,), (0,)), ((), ())), preferred_element_type=F32
    )
    summed = lax.psum_scatter(term, "rep", scatter_dimension=0, tiled=True)
    return (grad_pre, summed * factor)


def kernel(
    depth, near, far, most, order, factor,
    pre_hbm, w_hbm, cot_hbm, gp_hbm, gw_hbm,
    pre, pre_in, turned, w, cot, grad, gp,
    y_out, y_in, own, z_out, z_in, gw,
    s_local, s_pre_s, s_pre_r, s_near_s, s_near_r, s_x_s, s_x_r, s_fwd_s, s_fwd_r,
    s_y_s, s_y_r, s_z_s, s_z_r, s_gp,
):
    rep, fs, tp = lax.axis_index("rep"), lax.axis_index("fs"), lax.axis_index("tp")
    c, y, z = rep % CORES, (rep // CORES) % ROWS, rep // (CORES * ROWS)
    tokens, half = cot_hbm.shape
    hid = w_hbm.shape[0]
    block = own.shape[1]
    blocks = 2 * depth

    def at(z_, y_, c_, f_):
        return ((z_ * ROWS + y_) * CORES + c_, f_, tp)

    partner, across, beside = at(z, y, 1 - c, fs), at(z, y, c, 1 - fs), at(z, 1 - y, c, fs)

    def remote(src, dst, s, r, to):
        return pltpu.make_async_remote_copy(
            src_ref=src, dst_ref=dst, send_sem=s, recv_sem=r, device_id=to, device_id_type=MESH
        )

    def columns(i, c_):
        y_ = (1 - y) if i < depth else y
        k = (i % depth) * ROWS + y_
        return pl.ds(pl.multiple_of((k * CORES + c_) * block, block), block)

    def local(i, src, dst):
        return pltpu.make_async_copy(src, dst, s_local.at[i])

    loads = [local(0, pre_hbm, pre), local(1, cot_hbm, cot.at[0, pl.ds(0, tokens)]), local(2, w_hbm, w)]
    for l in loads:
        l.start()

    barrier = pltpu.get_barrier_semaphore()
    peers = [partner, across, beside]
    for d in range(1, depth):
        peers.append(at((z + d) % depth, y, c, fs))
    for p in peers:
        pl.semaphore_signal(barrier, inc=1, device_id=p, device_id_type=MESH)
    pl.semaphore_wait(barrier, len(peers))

    x_copies = []
    for q, (a, n) in enumerate(far):
        x_copies.append(remote(
            cot_hbm.at[:, pl.ds(a, n)], cot.at[1, pl.ds(0, tokens), pl.ds(a, n)],
            s_x_s.at[q], s_x_r.at[q], across))
    x_copies[0].start()
    pre_copies = []
    for i in range(blocks):
        pre_copies.append(remote(
            pre_hbm.at[:, columns(i, 1 - c)], pre_in.at[i], s_pre_s.at[i], s_pre_r.at[i], partner))
        pre_copies[-1].start()
    near_copies = []
    for q, (a, n) in enumerate(near):
        near_copies.append(remote(
            cot_hbm.at[:, pl.ds(a, n)], cot.at[0, pl.ds(tokens, tokens), pl.ds(a, n)],
            s_near_s.at[q], s_near_r.at[q], partner))
        near_copies[-1].start()
    for xc in x_copies[1:]:
        xc.start()

    def turn(v):
        p = jnp.maximum(v.astype(F32), 0.0)
        return (p * p).T.astype(BF16)

    strip = 256

    def turn_own(first):
        for i in range(first, first + depth):
            cols = columns(i, c)

            @pl.loop(0, tokens // strip)
            def _(t):
                rows = pl.ds(pl.multiple_of(t * strip, strip), strip)
                turned[pl.ds(i * block, block), rows] = turn(pre[rows, cols])

    def turn_in(first):
        for i in range(first, first + depth):
            pre_copies[i].wait_recv()

        @pl.loop(first, first + depth)
        def _(i):
            @pl.loop(0, tokens // strip)
            def _(t):
                rows = pl.ds(pl.multiple_of(t * strip, strip), strip)
                to = pl.ds(pl.multiple_of(tokens + t * strip, strip), strip)
                turned[pl.ds(pl.multiple_of(i * block, block), block), to] = turn(pre_in[i, rows, :])

    tall = 2 * block

    chunks = [(0, a, n) for a, n in near] + [(1, a, n) for a, n in far]

    def span(h, a, n):
        return pl.ds(h * half + a, n)

    def y_copy(j):
        h, a, n = chunks[j]
        s = span(h, a, n)
        return remote(y_out.at[:, :, s], y_in.at[:, :, s], s_y_s.at[j], s_y_r.at[j], beside)

    slots, far_end = depth, depth - 1
    inner = (z > 0) & (z < far_end)

    def relayed(j):
        return j < len(chunks) - 2

    def z_copy(j, kind):
        h, a, n = chunks[j]
        s = span(h, a, n)
        if kind == "up":
            ends = (z == far_end) if relayed(j) else False
            block_, slot, to = jnp.where(ends, 0, (z + 1) % depth), jnp.where(ends, 3, 0), jnp.where(ends, far_end - 1, (z + 1) % depth)
        elif kind == "down":
            ends = (z == 0) if relayed(j) else False
            block_, slot, to = jnp.where(ends, far_end, (z + far_end) % depth), jnp.where(ends, 3, 2), jnp.where(ends, 1, (z + far_end) % depth)
        else:
            block_, slot, to = (z + 2) % depth, 1, (z + 2) % depth
        return remote(
            z_out.at[block_, :, s], z_in.at[slot, :, s],
            s_z_s.at[j * slots + slot], s_z_r.at[j * slots + slot], at(to, y, c, fs))

    def z_arrival(j, slot):
        h, a, n = chunks[j]
        s = span(h, a, n)
        return remote(
            z_out.at[0, :, s], z_in.at[slot, :, s],
            s_z_s.at[j * slots + slot], s_z_r.at[j * slots + slot], beside)

    def fwd_copy(q):
        a, n = far[q]
        return remote(
            cot.at[1, pl.ds(0, tokens), pl.ds(a, n)], cot.at[1, pl.ds(tokens, tokens), pl.ds(a, n)],
            s_fwd_s.at[q], s_fwd_r.at[q], partner)

    def product(j, mine):
        h, a, n = chunks[j]
        s = span(h, a, n)

        def dot(m):
            rows = pl.ds(pl.multiple_of(m * tall, tall), tall)
            return lax.dot_general(
                turned[rows, :], cot[h, :, pl.ds(a, n)], (((1,), (0,)), ((), ())),
                preferred_element_type=F32).reshape(2, block, n)

        if mine:

            @pl.loop(0, depth // 2)
            def _(m):
                own[pl.ds(m * 2, 2), :, s] = dot(m + depth // 2)
        else:

            @pl.loop(0, depth // 2)
            def _(m):
                y_out[pl.ds(m * 2, 2), :, s] = dot(m).astype(BF16)

            y_copy(j).start()

    def second(j):
        h, a, n = chunks[j]
        s = span(h, a, n)
        y_copy(j).wait_recv()

        @pl.loop(0, depth)
        def _(k):
            v = own[k, :, s] + y_in[k, :, s].astype(F32)
            own[k, :, s] = v
            z_out[k, :, s] = v.astype(BF16)

        z_copy(j, "up").start()
        z_copy(j, "down").start()

        if relayed(j):

            @pl.when(jnp.logical_not(inner))
            def _():
                z_copy(j, "two").start()
        else:
            z_copy(j, "two").start()

    def third(j):
        h, a, n = chunks[j]
        s = span(h, a, n)

        @pl.when(inner)
        def _():
            z_arrival(j, 3).wait_recv()
            to = (z + 2) % depth
            z_out[to, :, s] = (own[to, :, s] + z_in[3, :, s].astype(F32)).astype(BF16)
            z_copy(j, "two").start()

    def last(j):
        h, a, n = chunks[j]
        s = span(h, a, n)
        for slot, there in ((0, z > 0), (2, z < far_end), (1, None)) if relayed(j) else ((0, None), (2, None), (1, None)):

            def add(slot=slot):
                z_arrival(j, slot).wait_recv()
                own[z, :, s] = own[z, :, s] + z_in[slot, :, s].astype(F32)

            if there is None:
                add()
            else:
                pl.when(there)(add)
        place = pl.multiple_of((fs if h == 0 else 1 - fs) * half + a, 128)
        gw[:, pl.ds(place, n)] = own[z, :, s] * factor

    tm, tn = 256, 512

    def grad_tile(h, a, n, m, k):
        rows = pl.ds(pl.multiple_of(m * tm, tm), tm)
        outs = pl.ds(pl.multiple_of(k * tn, tn), tn)
        place = pl.multiple_of((fs if h == 0 else 1 - fs) * half + a, 128)
        return rows, outs, lax.dot_general(
            cot[h, rows, pl.ds(a, n)], w[outs, pl.ds(place, n)], (((1,), (1,)), ((), ())),
            preferred_element_type=F32)

    def grad_first(m):
        @pl.loop(0, hid // tn)
        def _(k):
            rows, outs, v = grad_tile(0, 0, half, m, k)
            grad[rows, outs] = v

    def grad_next(m):
        @pl.loop(0, hid // tn)
        def _(k):
            rows, outs, v = grad_tile(1, 0, most, m, k)
            grad[rows, outs] += v

    def gp_copy(m):
        rows = pl.ds(m * tm, tm)
        return pltpu.make_async_copy(gp.at[rows], gp_hbm.at[rows], s_gp.at[m])

    def grad_rest(m):
        @pl.loop(0, hid // tn)
        def _(k):
            rows, outs, v = grad_tile(1, most, half - most, m, k)
            p = jnp.maximum(pre[rows, outs].astype(F32), 0.0)
            gp[rows, outs] = ((grad[rows, outs] + v) * 2.0 * p).astype(BF16)

        gp_copy(m).start()

    def near_in(q):
        near_copies[q].wait_recv()

    def far_in(q):
        x_copies[q].wait_recv()
        fwd_copy(q).start()

    def far_both(q):
        fwd_copy(q).wait_recv()

    nn, nf = len(near), len(far)
    total = nn + nf
    steps = {
        "A": lambda j: product(j, False), "B": lambda j: product(j, True),
        "s": second, "t": third, "l": last, "n": near_in, "x": far_in, "f": far_both,
        "g": grad_first, "h": grad_next, "e": grad_rest, "o": turn_own, "i": turn_in,
    }
    loads[0].wait()
    turn_own(0)
    loads[1].wait()
    loads[2].wait()
    turn_in(0)
    for step in " ".join(order).split():
        steps[step[0]](int(step[1:]))
    out = local(3, gw, gw_hbm)
    out.start()

    for copy in pre_copies + near_copies + x_copies:
        copy.wait_send()
    for q in range(nf):
        fwd_copy(q).wait_send()
    for j in range(total):
        y_copy(j).wait_send()
        for kind in ("up", "down", "two"):
            z_copy(j, kind).wait_send()
    for m in range(tokens // tm):
        gp_copy(m).wait()
    out.wait()


def solution(mesh):
    reps, fs, tp = mesh.shape["rep"], mesh.shape["fs"], mesh.shape["tp"]
    depth = reps // (CORES * ROWS)

    def on_device(pre_act, down_weight, cotangent):
        tokens, hid = pre_act.shape
        half = cotangent.shape[1]
        width = down_weight.shape[1]
        block = hid // reps
        if not (fs == 2 and tp == 1 and depth * CORES * ROWS == reps and depth == 4
                and block % 128 == 0 and half % 1024 == 0 and hid % 512 == 0 and tokens == 1024):
            return plain(pre_act, down_weight, cotangent)
        step = half // 4
        near = chunks_of(half, [step] * 4)
        far = chunks_of(half, [step] * 3 + [step // 2] * 2)
        nn, nf = len(near), len(far)
        total = nn + nf
        factor = 1.0 / float(tokens * reps) ** 0.5
        dma = lambda n: pltpu.SemaphoreType.DMA((n,))
        vm = pltpu.VMEM
        return pl.pallas_call(
            functools.partial(kernel, depth, near, far, step * 2, ORDER, factor),
            out_shape=[
                jax.ShapeDtypeStruct((tokens, hid), BF16),
                jax.ShapeDtypeStruct((block, width), F32),
            ],
            in_specs=[pl.BlockSpec(memory_space=pl.ANY)] * 3,
            out_specs=[pl.BlockSpec(memory_space=pl.ANY)] * 2,
            scratch_shapes=[
                vm((tokens, hid), BF16),
                vm((2 * depth, tokens, block), BF16),
                vm((2 * depth * block, 2 * tokens), BF16),
                vm(down_weight.shape, BF16),
                vm((2, 2 * tokens, half), BF16),
                vm((tokens, hid), F32),
                vm((tokens, hid), BF16),
                vm((depth, block, width), BF16),
                vm((depth, block, width), BF16),
                vm((depth, block, width), F32),
                vm((depth, block, width), BF16),
                vm((depth, block, width), BF16),
                vm((block, width), F32),
                dma(4), dma(2 * depth), dma(2 * depth), dma(nn), dma(nn), dma(nf), dma(nf), dma(nf), dma(nf),
                dma(total), dma(total), dma(total * depth), dma(total * depth),
                dma(tokens // 256),
            ],
            compiler_params=pltpu.CompilerParams(
                collective_id=0, has_side_effects=True, vmem_limit_bytes=66 * 1000 * 1000
            ),
            cost_estimate=pl.CostEstimate(
                flops=8 * tokens * hid * width // 2, bytes_accessed=40 * 1024 * 1024, transcendentals=0),
        )(pre_act, down_weight, cotangent)

    return jax.shard_map(
        on_device,
        mesh=mesh,
        in_specs=(P("rep", ("fs", "tp")), P(("fs", "tp"), None), P("rep", ("fs", "tp"))),
        out_specs=(P("rep", ("fs", "tp")), P(("fs", "tp", "rep"), None)),
        check_vma=False,
    )
```

```python
import functools

import jax
import jax.numpy as jnp
from jax import lax
from jax.experimental import pallas as pl
from jax.experimental.pallas import tpu as pltpu
from jax.sharding import PartitionSpec as P

MESH = pl.DeviceIdType.MESH
CORES, ROWS = 2, 2
F32, BF16 = jnp.float32, jnp.bfloat16


ORDER = (
    "n0 A0 n1 A1",
    "o4 i4 B0 B1",
    "n2 A2 n3 A3",
    "s0 B2 x0 B3",
    "f0 A4 B4 s1",
    "g0 g1 t0 g2",
    "x1 s2 f1 A5",
    "B5 g3 t1 h0",
    "h1 s3 h2 t2",
    "h3 x2 s4 l0",
    "f2 A6 B6 t3",
    "s5 l1 x3 t4",
    "f3 A7 B7 t5",
    "l2 x4 s6 f4",
    "A8 B8 s7 e0",
    "t6 l3 e1 s8",
    "l4 e2 l5 e3",
    "l6 l7 l8",
)


def chunks_of(width, sizes):
    out, at = [], 0
    for s in sizes:
        out.append((at, s))
        at += s
    assert at == width
    return out


def plain(pre_act, down_weight, cotangent):
    whole = lax.all_gather(cotangent, ("fs", "tp"), axis=1, tiled=True)
    grad_hidden = lax.dot_general(
        whole, down_weight, (((1,), (1,)), ((), ())), preferred_element_type=F32
    )
    positive = jnp.maximum(pre_act.astype(F32), 0.0)
    grad_pre = (grad_hidden * 2.0 * positive).astype(BF16)
    hidden = (positive * positive).astype(BF16)
    factor = 1.0 / jnp.sqrt(jnp.float32(pre_act.shape[0] * lax.axis_size("rep")))
    term = lax.dot_general(
        hidden, whole, (((0,), (0,)), ((), ())), preferred_element_type=F32
    )
    summed = lax.psum_scatter(term, "rep", scatter_dimension=0, tiled=True)
    return (grad_pre, summed * factor)


def kernel(
    depth, near, far, most, order, factor,
    pre_hbm, w_hbm, cot_hbm, gp, gw,
    pre, pre_in, turned, w, cot, grad,
    y_out, y_in, own, z_out, z_in,
    s_local, s_pre_s, s_pre_r, s_near_s, s_near_r, s_x_s, s_x_r, s_fwd_s, s_fwd_r,
    s_y_s, s_y_r, s_z_s, s_z_r,
):
    rep, fs, tp = lax.axis_index("rep"), lax.axis_index("fs"), lax.axis_index("tp")
    c, y, z = rep % CORES, (rep // CORES) % ROWS, rep // (CORES * ROWS)
    tokens, half = cot_hbm.shape
    hid = w_hbm.shape[0]
    block = own.shape[1]
    blocks = 2 * depth

    def at(z_, y_, c_, f_):
        return ((z_ * ROWS + y_) * CORES + c_, f_, tp)

    partner, across, beside = at(z, y, 1 - c, fs), at(z, y, c, 1 - fs), at(z, 1 - y, c, fs)

    def remote(src, dst, s, r, to):
        return pltpu.make_async_remote_copy(
            src_ref=src, dst_ref=dst, send_sem=s, recv_sem=r, device_id=to, device_id_type=MESH
        )

    def columns(i, c_):
        y_ = (1 - y) if i < depth else y
        k = (i % depth) * ROWS + y_
        return pl.ds(pl.multiple_of((k * CORES + c_) * block, block), block)

    def local(i, src, dst):
        return pltpu.make_async_copy(src, dst, s_local.at[i])

    loads = [local(0, pre_hbm, pre), local(1, cot_hbm, cot.at[0, pl.ds(0, tokens)]), local(2, w_hbm, w)]
    for l in loads:
        l.start()

    barrier = pltpu.get_barrier_semaphore()
    peers = [partner, across, beside]
    for d in range(1, depth):
        peers.append(at((z + d) % depth, y, c, fs))
    for p in peers:
        pl.semaphore_signal(barrier, inc=1, device_id=p, device_id_type=MESH)
    pl.semaphore_wait(barrier, len(peers))

    x_copies = []
    for q, (a, n) in enumerate(far):
        x_copies.append(remote(
            cot_hbm.at[:, pl.ds(a, n)], cot.at[1, pl.ds(0, tokens), pl.ds(a, n)],
            s_x_s.at[q], s_x_r.at[q], across))
    x_copies[0].start()
    pre_copies = []
    for i in range(blocks):
        pre_copies.append(remote(
            pre_hbm.at[:, columns(i, 1 - c)], pre_in.at[i], s_pre_s.at[i], s_pre_r.at[i], partner))
    near_copies = []
    for q, (a, n) in enumerate(near):
        near_copies.append(remote(
            cot_hbm.at[:, pl.ds(a, n)], cot.at[0, pl.ds(tokens, tokens), pl.ds(a, n)],
            s_near_s.at[q], s_near_r.at[q], partner))
    for group in (pre_copies[:depth], near_copies[:2], pre_copies[depth:], near_copies[2:]):
        for copy in group:
            copy.start()
    for xc in x_copies[1:]:
        xc.start()

    def turn(v):
        p = jnp.maximum(v.astype(F32), 0.0)
        return (p * p).T.astype(BF16)

    strip = 256

    def turn_own(first):
        for i in range(first, first + depth):
            cols = columns(i, c)

            @pl.loop(0, tokens // strip)
            def _(t):
                rows = pl.ds(pl.multiple_of(t * strip, strip), strip)
                turned[pl.ds(i * block, block), rows] = turn(pre[rows, cols])

    def turn_in(first):
        for i in range(first, first + depth):
            pre_copies[i].wait_recv()

        @pl.loop(first, first + depth)
        def _(i):
            @pl.loop(0, tokens // strip)
            def _(t):
                rows = pl.ds(pl.multiple_of(t * strip, strip), strip)
                to = pl.ds(pl.multiple_of(tokens + t * strip, strip), strip)
                turned[pl.ds(pl.multiple_of(i * block, block), block), to] = turn(pre_in[i, rows, :])

    tall = 2 * block

    chunks = [(0, a, n) for a, n in near] + [(1, a, n) for a, n in far]

    def span(h, a, n):
        return pl.ds(h * half + a, n)

    def y_copy(j):
        h, a, n = chunks[j]
        s = span(h, a, n)
        return remote(y_out.at[:, :, s], y_in.at[:, :, s], s_y_s.at[j], s_y_r.at[j], beside)

    slots, far_end = depth, depth - 1
    inner = (z > 0) & (z < far_end)

    def relayed(j):
        return j < len(chunks) - 2

    def z_copy(j, kind):
        h, a, n = chunks[j]
        s = span(h, a, n)
        if kind == "up":
            ends = (z == far_end) if relayed(j) else False
            block_, slot, to = jnp.where(ends, 0, (z + 1) % depth), jnp.where(ends, 3, 0), jnp.where(ends, far_end - 1, (z + 1) % depth)
        elif kind == "down":
            ends = (z == 0) if relayed(j) else False
            block_, slot, to = jnp.where(ends, far_end, (z + far_end) % depth), jnp.where(ends, 3, 2), jnp.where(ends, 1, (z + far_end) % depth)
        else:
            block_, slot, to = (z + 2) % depth, 1, (z + 2) % depth
        return remote(
            z_out.at[block_, :, s], z_in.at[slot, :, s],
            s_z_s.at[j * slots + slot], s_z_r.at[j * slots + slot], at(to, y, c, fs))

    def z_arrival(j, slot):
        h, a, n = chunks[j]
        s = span(h, a, n)
        return remote(
            z_out.at[0, :, s], z_in.at[slot, :, s],
            s_z_s.at[j * slots + slot], s_z_r.at[j * slots + slot], beside)

    def fwd_copy(q):
        a, n = far[q]
        return remote(
            cot.at[1, pl.ds(0, tokens), pl.ds(a, n)], cot.at[1, pl.ds(tokens, tokens), pl.ds(a, n)],
            s_fwd_s.at[q], s_fwd_r.at[q], partner)

    def product(j, mine):
        h, a, n = chunks[j]
        s = span(h, a, n)

        def dot(m):
            rows = pl.ds(pl.multiple_of(m * tall, tall), tall)
            return lax.dot_general(
                turned[rows, :], cot[h, :, pl.ds(a, n)], (((1,), (0,)), ((), ())),
                preferred_element_type=F32).reshape(2, block, n)

        if mine:

            @pl.loop(0, depth // 2)
            def _(m):
                own[pl.ds(m * 2, 2), :, s] = dot(m + depth // 2)
        else:

            @pl.loop(0, depth // 2)
            def _(m):
                y_out[pl.ds(m * 2, 2), :, s] = dot(m).astype(BF16)

            y_copy(j).start()

    def second(j):
        h, a, n = chunks[j]
        s = span(h, a, n)
        y_copy(j).wait_recv()

        @pl.loop(0, depth)
        def _(k):
            v = own[k, :, s] + y_in[k, :, s].astype(F32)
            own[k, :, s] = v
            z_out[k, :, s] = v.astype(BF16)

        z_copy(j, "up").start()
        z_copy(j, "down").start()

        if relayed(j):

            @pl.when(jnp.logical_not(inner))
            def _():
                z_copy(j, "two").start()
        else:
            z_copy(j, "two").start()

    def third(j):
        h, a, n = chunks[j]
        s = span(h, a, n)

        @pl.when(inner)
        def _():
            z_arrival(j, 3).wait_recv()
            to = (z + 2) % depth
            z_out[to, :, s] = (own[to, :, s] + z_in[3, :, s].astype(F32)).astype(BF16)
            z_copy(j, "two").start()

    def last(j):
        h, a, n = chunks[j]
        s = span(h, a, n)
        for slot, there in ((0, z > 0), (2, z < far_end), (1, None)) if relayed(j) else ((0, None), (2, None), (1, None)):

            def add(slot=slot):
                z_arrival(j, slot).wait_recv()
                own[z, :, s] = own[z, :, s] + z_in[slot, :, s].astype(F32)

            if there is None:
                add()
            else:
                pl.when(there)(add)
        place = pl.multiple_of((fs if h == 0 else 1 - fs) * half + a, 128)
        gw[:, pl.ds(place, n)] = own[z, :, s] * factor

    tm, tn = 256, 512

    def grad_tile(h, a, n, m, k):
        rows = pl.ds(pl.multiple_of(m * tm, tm), tm)
        outs = pl.ds(pl.multiple_of(k * tn, tn), tn)
        place = pl.multiple_of((fs if h == 0 else 1 - fs) * half + a, 128)
        return rows, outs, lax.dot_general(
            cot[h, rows, pl.ds(a, n)], w[outs, pl.ds(place, n)], (((1,), (1,)), ((), ())),
            preferred_element_type=F32)

    def grad_first(m):
        if m == 0:
            loads[2].wait()

        @pl.loop(0, hid // tn)
        def _(k):
            rows, outs, v = grad_tile(0, 0, half, m, k)
            grad[rows, outs] = v

    def grad_next(m):
        @pl.loop(0, hid // tn)
        def _(k):
            rows, outs, v = grad_tile(1, 0, most, m, k)
            grad[rows, outs] += v

    def grad_rest(m):
        @pl.loop(0, hid // tn)
        def _(k):
            rows, outs, v = grad_tile(1, most, half - most, m, k)
            p = jnp.maximum(pre[rows, outs].astype(F32), 0.0)
            gp[rows, outs] = ((grad[rows, outs] + v) * 2.0 * p).astype(BF16)

    def near_in(q):
        near_copies[q].wait_recv()

    def far_in(q):
        x_copies[q].wait_recv()
        fwd_copy(q).start()

    def far_both(q):
        fwd_copy(q).wait_recv()

    nn, nf = len(near), len(far)
    total = nn + nf
    steps = {
        "A": lambda j: product(j, False), "B": lambda j: product(j, True),
        "s": second, "t": third, "l": last, "n": near_in, "x": far_in, "f": far_both,
        "g": grad_first, "h": grad_next, "e": grad_rest, "o": turn_own, "i": turn_in,
    }
    loads[0].wait()
    turn_own(0)
    loads[1].wait()
    turn_in(0)
    for step in " ".join(order).split():
        steps[step[0]](int(step[1:]))

    for copy in pre_copies + near_copies + x_copies:
        copy.wait_send()
    for q in range(nf):
        fwd_copy(q).wait_send()
    for j in range(total):
        y_copy(j).wait_send()
        for kind in ("up", "down", "two"):
            z_copy(j, kind).wait_send()


def solution(mesh):
    reps, fs, tp = mesh.shape["rep"], mesh.shape["fs"], mesh.shape["tp"]
    depth = reps // (CORES * ROWS)

    def on_device(pre_act, down_weight, cotangent):
        tokens, hid = pre_act.shape
        half = cotangent.shape[1]
        width = down_weight.shape[1]
        block = hid // reps
        if not (fs == 2 and tp == 1 and depth * CORES * ROWS == reps and depth == 4
                and block % 128 == 0 and half % 1024 == 0 and hid % 512 == 0 and tokens == 1024):
            return plain(pre_act, down_weight, cotangent)
        step = half // 4
        near = chunks_of(half, [step] * 4)
        far = chunks_of(half, [step] * 3 + [step // 2] * 2)
        nn, nf = len(near), len(far)
        total = nn + nf
        factor = 1.0 / float(tokens * reps) ** 0.5
        dma = lambda n: pltpu.SemaphoreType.DMA((n,))
        vm = pltpu.VMEM
        return pl.pallas_call(
            functools.partial(kernel, depth, near, far, step * 2, ORDER, factor),
            out_shape=[
                pltpu.VMEM((tokens, hid), BF16),
                pltpu.VMEM((block, width), F32),
            ],
            in_specs=[pl.BlockSpec(memory_space=pl.ANY)] * 3,
            out_specs=[pl.BlockSpec(memory_space=pltpu.VMEM)] * 2,
            scratch_shapes=[
                vm((tokens, hid), BF16),
                vm((2 * depth, tokens, block), BF16),
                vm((2 * depth * block, 2 * tokens), BF16),
                vm(down_weight.shape, BF16),
                vm((2, 2 * tokens, half), BF16),
                vm((tokens, hid), F32),
                vm((depth, block, width), BF16),
                vm((depth, block, width), BF16),
                vm((depth, block, width), F32),
                vm((depth, block, width), BF16),
                vm((depth, block, width), BF16),
                dma(4), dma(2 * depth), dma(2 * depth), dma(nn), dma(nn), dma(nf), dma(nf), dma(nf), dma(nf),
                dma(total), dma(total), dma(total * depth), dma(total * depth),
            ],
            compiler_params=pltpu.CompilerParams(
                collective_id=0, has_side_effects=True, vmem_limit_bytes=54 * 1024 * 1024
            ),
            cost_estimate=pl.CostEstimate(
                flops=8 * tokens * hid * width // 2, bytes_accessed=40 * 1024 * 1024, transcendentals=0),
        )(pre_act, down_weight, cotangent)

    return jax.shard_map(
        on_device,
        mesh=mesh,
        in_specs=(P("rep", ("fs", "tp")), P(("fs", "tp"), None), P("rep", ("fs", "tp"))),
        out_specs=(P("rep", ("fs", "tp")), P(("fs", "tp", "rep"), None)),
        check_vma=False,
    )
```
